32 devices in a mesh: sp: 16 (over z, y, core), tp: 2 (over x).
Axes of the slice: x: 2, y: 2, z: 4, core: 2. Of those that a mesh axis runs over, the one named last changes fastest.
Arguments:
- glu_value: bfloat16 [8192, 1024], P('sp', 'tp'), may hold values from -6 to 6
- glu_gate: bfloat16 [8192, 1024], P('sp', 'tp'), may hold values from -8 to 8
- conv_taps: float32 [31, 1024], P(None, 'tp'), may hold values from -1 to 1
- channel_norm_gain: float32 [1024], P('tp'), may hold values from 0.1 to 1.9
- channel_norm_bias: float32 [1024], P('tp'), may hold values from -3 to 3
- out_proj: bfloat16 [1024, 2048], P('tp'), may hold values from -0.1875 to 0.1875
- out_grad: bfloat16 [8192, 2048], P('sp'), may hold values from -6 to 6
Outputs:
- grad_value: bfloat16 [8192, 1024], P('sp', 'tp')
- grad_gate: bfloat16 [8192, 1024], P('sp', 'tp')
- grad_taps: float32 [31, 1024], P(None, 'tp')
- norm_gain_gradient: float32 [1024], P('tp')
- grad_bias: float32 [1024], P('tp')
- grad_proj: float32 [2048, 1024], P('sp', 'tp')
The draws below stay inside these ranges and needn't reach their ends.
All inputs are finite; a program needn't handle non-finite values.
Results may differ from the reference program's by a relative error of at most 0.0049.
Values may be sent and summed in bfloat16 or wider, within the bound.
No kernel may reach another device: no remote copies, remote signals or barrier semaphores. Data moves between devices by JAX's collectives and lax.ppermute only.
A program may use at most 64 MiB of HBM per device.

```python
import jax
import jax.numpy as jnp
from jax import lax

D = 2048
CONV_CHANNELS = 1024
TAPS = 31
TOK_DEV = 512
SEQ = 8192


def spiked(result, rng, source, target, blocks, factor):
    def block_of(position):
        return (jnp.arange(result.shape[position]) // (result.shape[position] // blocks)).reshape((-1,) + (1,) * (result.ndim - 1 - position))

    one_side = jax.random.permutation(rng, blocks)[block_of(target)]
    far = (block_of(target) + blocks // 2) % blocks
    return jnp.where((block_of(source) == one_side) | (block_of(source) == far), factor * result, result)


def block_scale(own_key, dims, split, least, top_value):
    level, own = 1.0, jax.random.fold_in(own_key, 6)
    for dim, blocks in split:
        draws = jnp.exp(jax.random.uniform(jax.random.fold_in(own, dim), (blocks,), jnp.float32, least / len(split), top_value / len(split)))
        level = level * jnp.repeat(draws, dims[dim] // blocks).reshape([-1 if axis == dim else 1 for axis in range(len(dims))])
    return level


def gaussian(own_key, extent, deviation, limit, split=(), kind=jnp.bfloat16):
    values = deviation * jax.random.normal(own_key, extent, jnp.float32)
    if split:
        values = values * block_scale(own_key, extent, split, -0.22, 0.18)
    return jnp.clip(values, -limit, limit).astype(kind)


def gaussian_with(stream_key, extent, scale, most, pieces, heavy, held_as=jnp.bfloat16):
    result = scale * jax.random.normal(stream_key, extent, jnp.float32)
    if pieces:
        result = result * block_scale(stream_key, extent, pieces, -0.22, 0.18)
    return jnp.clip(spiked(result, jax.random.fold_in(stream_key, 3), *heavy), -most, most).astype(held_as)


def setup_inputs(seed: int = 0) -> dict:
    arg_keys = jax.random.split(jax.random.key(seed), 8)
    glu_value = gaussian(arg_keys[0], (SEQ, CONV_CHANNELS), 1.0, 6.0, ((0, 16), (1, 2)))
    glu_gate = gaussian(arg_keys[1], (SEQ, CONV_CHANNELS), 1.5, 8.0, ((0, 16), (1, 2)))
    conv_taps = gaussian(arg_keys[2], (TAPS, CONV_CHANNELS), TAPS ** -0.5, 1.0, ((1, 2),), jnp.float32)
    channel_norm_gain = jnp.clip(1.0 + 0.18 * jax.random.normal(arg_keys[3], (CONV_CHANNELS,), jnp.float32), 0.1, 1.9)
    channel_norm_bias = gaussian(arg_keys[4], (CONV_CHANNELS,), 0.5, 3.0, ((0, 2),), jnp.float32)
    out_proj = gaussian(arg_keys[5], (CONV_CHANNELS, D), CONV_CHANNELS ** -0.5, 0.1875, ((0, 2),))
    out_grad = gaussian_with(arg_keys[6], (SEQ, D), 1.0, 6.0, ((0, 16),), (0, 1, 16, 2.0))
    return dict(glu_value=glu_value, glu_gate=glu_gate, conv_taps=conv_taps, channel_norm_gain=channel_norm_gain, channel_norm_bias=channel_norm_bias, out_proj=out_proj, out_grad=out_grad)


def rows_at(array, first, count, length):
    index = first + jnp.arange(count, dtype=jnp.int32)
    valid = jnp.logical_and(index >= 0, index < length)
    taken = jnp.take(array, jnp.clip(index, 0, length - 1), axis=0)
    return jnp.where(valid[:, None], taken, jnp.zeros_like(taken))

def reference(glu_value, glu_gate, conv_taps, channel_norm_gain, channel_norm_bias, out_proj, out_grad):
    length = glu_value.shape[0]
    blocks = length // TOK_DEV
    span = TOK_DEV + TAPS - 1
    window = span + TAPS - 1

    def step(carry, block):
        proj_acc, taps_acc, gain_acc, bias_acc = carry
        first = (block * TOK_DEV).astype(jnp.int32)
        value = rows_at(glu_value, first - (TAPS - 1), window, length).astype(jnp.float32)
        sig_gate = jax.nn.sigmoid(rows_at(glu_gate, first - (TAPS - 1), window, length).astype(jnp.float32))
        gated = (value * sig_gate).astype(jnp.bfloat16).astype(jnp.float32)
        conv_output = jnp.zeros((span, CONV_CHANNELS), jnp.float32)
        for k in range(TAPS):
            conv_output = conv_output + conv_taps[k][None, :] * gated[k:k + span]
        channel_mean = lax.optimization_barrier(jnp.mean(conv_output, axis=1, keepdims=True))
        var = lax.optimization_barrier(jnp.mean(conv_output * conv_output, axis=1, keepdims=True)) - channel_mean * channel_mean
        inverse_deviation = lax.rsqrt(var + 1e-05)
        centered = (conv_output - channel_mean) * inverse_deviation
        normalized_rows = centered * channel_norm_gain[None, :] + channel_norm_bias[None, :]
        sig_norm = jax.nn.sigmoid(normalized_rows)
        act = (normalized_rows * sig_norm).astype(jnp.bfloat16)
        grad_rows = rows_at(out_grad, first, span, length)
        grad_act = jnp.dot(grad_rows, out_proj.T, preferred_element_type=jnp.float32)
        normalized_gradient = grad_act * sig_norm * (1.0 + normalized_rows * (1.0 - sig_norm))
        scaled_rows = normalized_gradient * channel_norm_gain[None, :]
        conv_gradient = inverse_deviation * (scaled_rows - lax.optimization_barrier(jnp.mean(scaled_rows, axis=1, keepdims=True)) - centered * lax.optimization_barrier(jnp.mean(scaled_rows * centered, axis=1, keepdims=True)))
        own_grad = conv_gradient[:TOK_DEV]
        proj_acc = proj_acc + jnp.dot(grad_rows[:TOK_DEV].T, act[:TOK_DEV], preferred_element_type=jnp.float32)
        gain_acc = gain_acc + lax.optimization_barrier(jnp.sum(normalized_gradient[:TOK_DEV] * centered[:TOK_DEV], axis=0))
        bias_acc = bias_acc + lax.optimization_barrier(jnp.sum(normalized_gradient[:TOK_DEV], axis=0))
        taps_acc = taps_acc + jnp.stack([lax.optimization_barrier(jnp.sum(own_grad * gated[k:k + TOK_DEV], axis=0)) for k in range(TAPS)], axis=0)
        grad_gated = jnp.zeros((TOK_DEV, CONV_CHANNELS), jnp.float32)
        for k in range(TAPS):
            grad_gated = grad_gated + conv_taps[k][None, :] * conv_gradient[TAPS - 1 - k:TAPS - 1 - k + TOK_DEV]
        own_value = value[TAPS - 1:TAPS - 1 + TOK_DEV]
        own_sig = sig_gate[TAPS - 1:TAPS - 1 + TOK_DEV]
        grad_value = (grad_gated * own_sig).astype(jnp.bfloat16)
        grad_gate = (grad_gated * own_value * own_sig * (1.0 - own_sig)).astype(jnp.bfloat16)
        return ((proj_acc, taps_acc, gain_acc, bias_acc), (grad_value, grad_gate))
    init = (jnp.zeros((D, CONV_CHANNELS), jnp.float32), jnp.zeros((TAPS, CONV_CHANNELS), jnp.float32), jnp.zeros((CONV_CHANNELS,), jnp.float32), jnp.zeros((CONV_CHANNELS,), jnp.float32))
    (grad_proj, grad_taps, norm_gain_gradient, grad_bias), (value_blocks, gate_blocks) = lax.scan(step, init, jnp.arange(blocks, dtype=jnp.int32))
    grad_value = value_blocks.reshape(length, CONV_CHANNELS)
    grad_gate = gate_blocks.reshape(length, CONV_CHANNELS)
    return (grad_value, grad_gate, grad_taps, norm_gain_gradient, grad_bias, grad_proj)
```

```python
import jax
import jax.numpy as jnp
import numpy as np
from jax import lax
from jax.experimental import pallas as pl
from jax.experimental.pallas import tpu as pltpu
from jax.sharding import PartitionSpec as P


def passed_along(shard, axis, by):
    size = lax.axis_size(axis)
    pairs = [(i, i + by) for i in range(size) if 0 <= i + by < size]
    return lax.ppermute(shard, axis, pairs)


def swapped(shard, axis, bit):
    size = lax.axis_size(axis)
    return lax.ppermute(shard, axis, [(i, i ^ (1 << bit)) for i in range(size)])


def bits_of(size):
    bits = size.bit_length() - 1
    return bits if 1 << bits == size else None


def summed_over(shard, axis):
    bits = bits_of(lax.axis_size(axis))
    if bits is None:
        return lax.psum(shard, axis)
    for bit in range(bits):
        shard = shard + swapped(shard, axis, bit)
    return shard


def together(*values):
    return lax.optimization_barrier(values)


def block_products(order, out_grad, act, block, kind):
    def body(order_ref, grad_ref, act_ref, out_ref):
        for n in range(order.shape[0]):
            first = pl.multiple_of(order_ref[n] * block, block)
            out_ref[n] = lax.dot_general(
                grad_ref[:, pl.ds(first, block)],
                act_ref[...],
                (((0,), (0,)), ((), ())),
                preferred_element_type=jnp.float32,
            ).astype(kind)

    vmem = pl.BlockSpec(memory_space=pltpu.VMEM)
    return pl.pallas_call(
        body,
        in_specs=[pl.BlockSpec(memory_space=pltpu.SMEM), vmem, vmem],
        out_specs=vmem,
        out_shape=jax.ShapeDtypeStruct((order.shape[0], block, act.shape[1]), kind),
    )(order, out_grad, act)


def halved(blocks, where, axis, bit):
    kept = lax.index_in_dim(blocks, 0, where, keepdims=False)
    sent = lax.index_in_dim(blocks, 1, where, keepdims=False)
    return kept, swapped(sent.astype(jnp.bfloat16), axis, bit)


def added(pair):
    return pair[0] + pair[1].astype(jnp.float32)


def on_device(
    glu_value, glu_gate, conv_taps, channel_norm_gain, channel_norm_bias, out_proj, out_grad
):
    rows, width = glu_value.shape
    taps = conv_taps.shape[0]
    channels = width * lax.axis_size("tp")
    size = lax.axis_size("sp")
    bits = bits_of(size)
    block = out_grad.shape[1] // size
    by_halves = bits == 4 and block % 128 == 0 and width % 256 == 0

    value = glu_value.astype(jnp.float32)
    sig_gate = jax.nn.sigmoid(glu_gate.astype(jnp.float32))
    gated = (value * sig_gate).astype(jnp.bfloat16)
    before = passed_along(gated[rows - (taps - 1) :], "sp", 1)
    grad_act = lax.dot_general(
        out_grad, out_proj, (((1,), (1,)), ((), ())), preferred_element_type=jnp.float32
    )
    before, grad_act = together(before, grad_act)
    padded = jnp.concatenate([before, gated], axis=0).astype(jnp.float32)
    conv_output = jnp.zeros((rows, width), jnp.float32)
    for k in range(taps):
        conv_output = conv_output + conv_taps[k][None, :] * padded[k : k + rows]
    sums = summed_over(
        jnp.stack([jnp.sum(conv_output, axis=1), jnp.sum(conv_output * conv_output, axis=1)]), "tp"
    )
    channel_mean = (sums[0] / channels)[:, None]
    var = (sums[1] / channels)[:, None] - channel_mean * channel_mean
    inverse_deviation = lax.rsqrt(var + 1e-05)
    centered_standardized = (conv_output - channel_mean) * inverse_deviation
    normalized_rows = (
        centered_standardized * channel_norm_gain[None, :] + channel_norm_bias[None, :]
    )
    sig_norm = jax.nn.sigmoid(normalized_rows)
    act = (normalized_rows * sig_norm).astype(jnp.bfloat16)
    normalized_gradient = grad_act * sig_norm * (1.0 + normalized_rows * (1.0 - sig_norm))
    scaled_rows = normalized_gradient * channel_norm_gain[None, :]
    row_terms = jnp.stack(
        [jnp.sum(scaled_rows, axis=1), jnp.sum(scaled_rows * centered_standardized, axis=1)]
    )
    column_terms = jnp.stack(
        [jnp.sum(normalized_gradient * centered_standardized, axis=0), jnp.sum(normalized_gradient, axis=0)]
    )
    if by_halves:
        relative = np.array(
            [sum(((n >> (bits - 2 - b)) & 1) << (b + 1) for b in range(bits - 1)) for n in range(size // 2)],
            np.int32,
        )
        me = lax.axis_index("sp").astype(jnp.int32)
        act, row_terms = together(act, row_terms)
        sent = block_products(jnp.asarray(relative + 1) ^ me, out_grad, act, block, jnp.bfloat16)
        got = swapped(sent, "sp", 0)
        kept = block_products(jnp.asarray(relative) ^ me, out_grad, act, block, jnp.float32)
        terms = summed_over(row_terms, "tp")
        got, kept, terms = together(got, kept, terms)
        blocks = added((kept, got)).reshape(2, 2, 2, block, width)
        left = halved(blocks[..., : width // 2], 0, "sp", 1)
        right = halved(blocks[..., width // 2 :], 1, "sp", 2)
    else:
        grad_proj = lax.psum_scatter(
            lax.dot_general(
                out_grad, act, (((0,), (0,)), ((), ())), preferred_element_type=jnp.float32
            ),
            "sp",
            scatter_dimension=0,
            tiled=True,
        )
        terms = summed_over(row_terms, "tp")
    conv_output_gradient = inverse_deviation * (
        scaled_rows
        - (terms[0] / channels)[:, None]
        - centered_standardized * (terms[1] / channels)[:, None]
    )
    ahead = passed_along(conv_output_gradient[: taps - 1], "sp", -1)
    taps_local = jnp.stack(
        [jnp.sum(conv_output_gradient * padded[k : k + rows], axis=0) for k in range(taps)], axis=0
    )
    summed = jnp.concatenate([taps_local, column_terms], axis=0)
    if by_halves:
        left, right, summed, ahead, conv_output_gradient = together(
            left, right, summed, ahead, conv_output_gradient
        )
        left = halved(added(left), 0, "sp", 2)
        right = halved(added(right), 0, "sp", 1)
        summed = (summed, swapped(summed, "sp", 0))

    def conv_back(source, count):
        total = jnp.zeros((count, width), jnp.float32)
        for k in range(taps):
            total = total + conv_taps[k][None, :] * source[taps - 1 - k : taps - 1 - k + count]
        return total

    after = jnp.concatenate([conv_output_gradient, ahead], axis=0)
    if by_halves:
        cut = rows // 2
        top = conv_back(after, cut)
        left, right, summed, top, after = together(left, right, summed, top, after)
        both = jnp.concatenate([added(left), added(right)], axis=-1)
        both = halved(both, 0, "sp", 3)
        summed = summed[0] + summed[1]
        summed = (summed, swapped(summed, "sp", 1))
        bottom = conv_back(after[cut:], rows - cut)
        both, summed, bottom = together(both, summed, bottom)
        grad_proj = added(both)
        summed = summed[0] + summed[1]
        for bit in (2, 3):
            summed = summed + swapped(summed, "sp", bit)
        grad_gated = jnp.concatenate([top, bottom], axis=0)
    else:
        summed = summed_over(summed, "sp")
        grad_gated = conv_back(after, rows)
    grad_value = (grad_gated * sig_gate).astype(jnp.bfloat16)
    grad_gate = (grad_gated * value * sig_gate * (1.0 - sig_gate)).astype(jnp.bfloat16)
    return (grad_value, grad_gate, summed[:taps], summed[taps], summed[taps + 1], grad_proj)


def solution(mesh):
    return jax.shard_map(
        on_device,
        mesh=mesh,
        in_specs=(
            P("sp", "tp"),
            P("sp", "tp"),
            P(None, "tp"),
            P("tp"),
            P("tp"),
            P("tp", None),
            P("sp", None),
        ),
        out_specs=(P("sp", "tp"), P("sp", "tp"), P(None, "tp"), P("tp"), P("tp"), P("sp", "tp")),
        check_vma=False,
    )
```

```python
import jax
import jax.numpy as jnp
import numpy as np
from jax import lax
from jax.experimental import pallas as pl
from jax.experimental.pallas import tpu as pltpu
from jax.sharding import PartitionSpec as P

LANES = 128
TILE = 64


def passed_along(shard, axis, by):
    size = lax.axis_size(axis)
    pairs = [(i, i + by) for i in range(size) if 0 <= i + by < size]
    return lax.ppermute(shard, axis, pairs)


def swapped(shard, axis, bit):
    size = lax.axis_size(axis)
    return lax.ppermute(shard, axis, [(i, i ^ (1 << bit)) for i in range(size)])


def bits_of(size):
    bits = size.bit_length() - 1
    return bits if 1 << bits == size else None


def summed_over(shard, axis):
    bits = bits_of(lax.axis_size(axis))
    if bits is None:
        return lax.psum(shard, axis)
    for bit in range(bits):
        shard = shard + swapped(shard, axis, bit)
    return shard


def together(*values):
    return lax.optimization_barrier(values)


def call(body, outs, *args, scalars=0, scratch=()):
    vmem = pl.BlockSpec(memory_space=pltpu.VMEM)
    return pl.pallas_call(
        body,
        in_specs=[pl.BlockSpec(memory_space=pltpu.SMEM)] * scalars + [vmem] * (len(args) - scalars),
        out_specs=[vmem] * len(outs),
        out_shape=[jax.ShapeDtypeStruct(shape, kind) for shape, kind in outs],
        scratch_shapes=list(scratch),
    )(*args)


def group(g):
    return slice(g * LANES, (g + 1) * LANES)


def as_row(columns):
    return jnp.sum(columns.T, axis=0, keepdims=True)


def as_column(row):
    return jnp.broadcast_to(row, (LANES, row.shape[1])).T


def conv_forward(value, gate, before, conv_taps):
    rows, width = value.shape
    taps = conv_taps.shape[0]
    pad = before.shape[0]
    groups = width // LANES

    def body(value_ref, gate_ref, before_ref, taps_ref, conv_ref, padded_ref, sums_ref):
        for g in range(groups):
            padded_ref[g, :pad, :] = before_ref[:, group(g)].astype(jnp.float32)
            v = value_ref[:, group(g)].astype(jnp.float32)
            s = jax.nn.sigmoid(gate_ref[:, group(g)].astype(jnp.float32))
            padded_ref[g, pad:, :] = (v * s).astype(jnp.bfloat16).astype(jnp.float32)
        for g in range(groups):
            weights = [taps_ref[k : k + 1, group(g)] for k in range(taps)]

            def tile(n, carry):
                first = pl.multiple_of(n * TILE, TILE)
                total = jnp.zeros((TILE, LANES), jnp.float32)
                for k in range(taps):
                    total = total + weights[k] * padded_ref[
                        g, pl.ds(first + (pad - taps + 1 + k), TILE), :
                    ]
                conv_ref[pl.ds(first, TILE), group(g)] = total
                return carry

            lax.fori_loop(0, rows // TILE, tile, 0)
        total = jnp.zeros((rows, LANES), jnp.float32)
        squares = jnp.zeros((rows, LANES), jnp.float32)
        for g in range(groups):
            c = conv_ref[:, group(g)]
            total = total + c
            squares = squares + c * c
        sums_ref[0:1, :] = as_row(total)
        sums_ref[1:2, :] = as_row(squares)

    return call(
        body,
        [
            ((rows, width), jnp.float32),
            ((groups, rows + pad, LANES), jnp.float32),
            ((2, rows), jnp.float32),
        ],
        value, gate, before, conv_taps,
    )


def statistics(sums_ref, channels):
    mean = sums_ref[0:1, :] / channels
    var = sums_ref[1:2, :] / channels - mean * mean
    return as_column(mean), as_column(lax.rsqrt(var + 1e-05))


def products(me_ref, order, grad_ref, act, block):
    for n in range(0, len(order), 2):
        picked = [
            grad_ref[:, pl.ds(pl.multiple_of((me_ref[0] ^ b) * block, block), block)]
            for b in order[n : n + 2]
        ]
        pair = jnp.dot(
            act, jnp.concatenate(picked, axis=1), preferred_element_type=jnp.float32
        )
        yield n, pair[:, :block]
        yield n + 1, pair[:, block:]


def normed_act(conv, sums, gain, bias, out_grad, me, order, block, channels):
    rows, width = conv.shape
    groups = width // LANES
    count = len(order)

    def body(me_ref, conv_ref, sums_ref, gain_ref, bias_ref, grad_ref, act_ref, sent_ref):
        mean, rstd = statistics(sums_ref, channels)
        for g in range(groups):
            xhat = (conv_ref[:, group(g)] - mean) * rstd
            normed = xhat * gain_ref[:, group(g)] + bias_ref[:, group(g)]
            act = normed * jax.nn.sigmoid(normed)
            act_ref[group(g), :] = act.T.astype(jnp.bfloat16)
        if count:
            for n, product in products(me_ref, order, grad_ref, act_ref[...], block):
                sent_ref[n] = product.astype(jnp.bfloat16)
        else:
            sent_ref[...] = jnp.zeros_like(sent_ref)

    shape = (count, width, block) if count else (16, LANES)
    return call(
        body,
        [((width, rows), jnp.bfloat16), (shape, jnp.bfloat16)],
        me, conv, sums, gain, bias, out_grad,
        scalars=1,
    )


def kept_products(act, out_grad, me, order, block, got):
    width = act.shape[0]
    half = width // 2
    count = len(order)

    def body(me_ref, act_ref, grad_ref, got_ref, kl_ref, sl_ref, kr_ref, sr_ref):
        for n, product in products(me_ref, order, grad_ref, act_ref[...], block):
            product = product + got_ref[n].astype(jnp.float32)
            left, right = product[:half], product[half:]
            first, second, rest = n >> 2, (n >> 1) & 1, n & 1
            if first:
                sl_ref[second * 2 + rest] = left.astype(jnp.bfloat16)
            else:
                kl_ref[second * 2 + rest] = left
            if second:
                sr_ref[first * 2 + rest] = right.astype(jnp.bfloat16)
            else:
                kr_ref[first * 2 + rest] = right

    shape = (count // 2, half, block)
    return call(
        body,
        [(shape, jnp.float32), (shape, jnp.bfloat16)] * 2,
        me, act, out_grad, got,
        scalars=1,
    )


def normed_gradient(conv, sums, gain, bias, upper, lower, channels):
    rows, width = conv.shape
    groups = width // LANES
    cut = upper.shape[0]

    def body(conv_ref, sums_ref, gain_ref, bias_ref, up_ref, low_ref, gx_ref, xhat_ref, row_ref, col_ref):
        mean, rstd = statistics(sums_ref, channels)
        first = jnp.zeros((rows, LANES), jnp.float32)
        second = jnp.zeros((rows, LANES), jnp.float32)
        for g in range(groups):
            xhat = (conv_ref[:, group(g)] - mean) * rstd
            normed = xhat * gain_ref[:, group(g)] + bias_ref[:, group(g)]
            sig = jax.nn.sigmoid(normed)
            ga = jnp.concatenate([up_ref[:, group(g)], low_ref[:, group(g)]], axis=0)
            gn = ga * sig * (1.0 + normed * (1.0 - sig))
            col_ref[0:1, group(g)] = jnp.sum(gn * xhat, axis=0, keepdims=True)
            col_ref[1:2, group(g)] = jnp.sum(gn, axis=0, keepdims=True)
            gx = gn * gain_ref[:, group(g)]
            first = first + gx
            second = second + gx * xhat
            gx_ref[:, group(g)] = gx
            xhat_ref[:, group(g)] = xhat
        row_ref[0:1, :] = as_row(first)
        row_ref[1:2, :] = as_row(second)

    return call(
        body,
        [
            ((rows, width), jnp.float32),
            ((rows, width), jnp.float32),
            ((2, rows), jnp.float32),
            ((2, width), jnp.float32),
        ],
        conv, sums, gain, bias, upper, lower,
    )


def conv_gradient(gx, xhat, sums, terms, channels, pad):
    rows, width = gx.shape
    groups = width // LANES

    def body(gx_ref, xhat_ref, sums_ref, terms_ref, out_ref, edge_ref):
        _, rstd = statistics(sums_ref, channels)
        first = as_column(terms_ref[0:1, :] / channels)
        second = as_column(terms_ref[1:2, :] / channels)
        for g in range(groups):
            out = rstd * (gx_ref[:, group(g)] - first - xhat_ref[:, group(g)] * second)
            out_ref[g] = out
            edge_ref[g] = out[:pad]

    return call(
        body,
        [((groups, rows, LANES), jnp.float32), ((groups, pad, LANES), jnp.float32)],
        gx, xhat, sums, terms,
    )


def taps_gradient(grad_conv, padded, columns, taps):
    groups, rows, _ = grad_conv.shape
    pad = padded.shape[1] - rows
    height = -(-(taps + 2) // 8) * 8

    def body(grad_ref, padded_ref, col_ref, out_ref):
        out_ref[...] = jnp.zeros_like(out_ref)
        out_ref[taps : taps + 2, :] = col_ref[...]
        for g in range(groups):
            def tile(n, totals):
                first = pl.multiple_of(n * 16, 16)
                grad = [grad_ref[g, pl.ds(first + 8 * m, 8), :] for m in range(2)]
                return tuple(
                    totals[k] + sum(
                        grad[m] * padded_ref[g, pl.ds(first + (8 * m + pad - taps + 1 + k), 8), :]
                        for m in range(2)
                    )
                    for k in range(taps)
                )

            totals = lax.fori_loop(
                0, rows // 16, tile, tuple(jnp.zeros((8, LANES), jnp.float32) for _ in range(taps))
            )
            for k in range(taps):
                out_ref[k : k + 1, group(g)] = jnp.sum(totals[k], axis=0, keepdims=True)

    return call(body, [((height, groups * LANES), jnp.float32)], grad_conv, padded, columns)[0]


def conv_backward(grad_conv, ahead, conv_taps, value, gate, start):
    groups, rows, _ = grad_conv.shape
    taps = conv_taps.shape[0]
    count = rows // 2
    width = groups * LANES
    final = ahead is not None

    def body(*refs):
        if final:
            grad_ref, ahead_ref, taps_ref, value_ref, gate_ref, gv_ref, gg_ref, held_ref = refs
            held_ref[:, :count, :] = grad_ref[:, start:, :]
            held_ref[:, count:, :] = ahead_ref[...]
            source, base = held_ref, 0
        else:
            grad_ref, taps_ref, value_ref, gate_ref, gv_ref, gg_ref = refs
            source, base = grad_ref, start
        for g in range(groups):
            weights = [taps_ref[k : k + 1, group(g)] for k in range(taps)]

            def tile(n, carry):
                first = pl.multiple_of(n * TILE, TILE)
                total = jnp.zeros((TILE, LANES), jnp.float32)
                for k in range(taps):
                    total = total + weights[k] * source[
                        g, pl.ds(first + (base + taps - 1 - k), TILE), :
                    ]
                here = pl.ds(first + start, TILE)
                v = value_ref[here, group(g)].astype(jnp.float32)
                s = jax.nn.sigmoid(gate_ref[here, group(g)].astype(jnp.float32))
                gv_ref[pl.ds(first, TILE), group(g)] = (total * s).astype(jnp.bfloat16)
                gg_ref[pl.ds(first, TILE), group(g)] = (total * v * s * (1.0 - s)).astype(jnp.bfloat16)
                return carry

            lax.fori_loop(0, count // TILE, tile, 0)

    outs = [((count, width), jnp.bfloat16)] * 2
    if final:
        scratch = [pltpu.VMEM((groups, count + ahead.shape[1], LANES), jnp.float32)]
        return call(body, outs, grad_conv, ahead, conv_taps, value, gate, scratch=scratch)
    return call(body, outs, grad_conv, conv_taps, value, gate)


def halved(blocks, axis, bit):
    count = blocks.shape[0] // 2
    return blocks[:count], swapped(blocks[count:].astype(jnp.bfloat16), axis, bit)


def added(pair):
    return pair[0] + pair[1].astype(jnp.float32)


def on_device(
    glu_value, glu_gate, conv_taps, channel_norm_gain, channel_norm_bias, out_proj, out_grad
):
    rows, width = glu_value.shape
    taps = conv_taps.shape[0]
    pad = -(-(taps - 1) // 16) * 16
    channels = width * lax.axis_size("tp")
    size = lax.axis_size("sp")
    bits = bits_of(size)
    block = out_grad.shape[1] // size
    by_halves = bits == 4 and block % LANES == 0 and width % 256 == 0
    gain, bias = channel_norm_gain[None, :], channel_norm_bias[None, :]
    cut = rows // 2
    me = lax.axis_index("sp").astype(jnp.int32).reshape(1)
    relative = []
    if by_halves:
        relative = [
            sum(((n >> (bits - 2 - b)) & 1) << (b + 1) for b in range(bits - 1))
            for n in range(size // 2)
        ]

    edge = (
        glu_value[rows - pad :].astype(jnp.float32)
        * jax.nn.sigmoid(glu_gate[rows - pad :].astype(jnp.float32))
    ).astype(jnp.bfloat16)
    before = passed_along(edge, "sp", 1)

    def act_gradient(part):
        return lax.dot_general(
            part, out_proj, (((1,), (1,)), ((), ())), preferred_element_type=jnp.float32
        )

    upper = act_gradient(out_grad[:cut])
    before, upper = together(before, upper)
    conv, padded, sums = conv_forward(glu_value, glu_gate, before, conv_taps)
    later, sums = together(out_grad, sums)
    lower = act_gradient(later[cut:])
    sums = summed_over(sums, "tp")
    sums, lower = together(sums, lower)
    act, sent = normed_act(
        conv, sums, gain, bias, out_grad, me, [r + 1 for r in relative], block, channels
    )
    if by_halves:
        got = swapped(sent, "sp", 0)
        sums, act = together(sums, act)
    gx, xhat, row_terms, column_terms = normed_gradient(
        conv, sums, gain, bias, upper, lower, channels
    )
    terms = summed_over(row_terms, "tp")
    if by_halves:
        got, row_terms = together(got, row_terms)
        kl, sl, kr, sr = kept_products(act, out_grad, me, relative, block, got)
        left = (kl, swapped(sl, "sp", 1))
        right = (kr, swapped(sr, "sp", 2))
        terms, kl = together(terms, kl)
        left = (kl, left[1])
    else:
        grad_proj = lax.psum_scatter(
            lax.dot_general(
                out_grad, act, (((0,), (1,)), ((), ())), preferred_element_type=jnp.float32
            ),
            "sp",
            scatter_dimension=0,
            tiled=True,
        )
    grad_conv, edge_gradient = conv_gradient(gx, xhat, sums, terms, channels, pad)
    ahead = passed_along(edge_gradient, "sp", -1)
    summed = taps_gradient(grad_conv, padded, column_terms, taps)
    if by_halves:
        left, right, summed, grad_conv = together(left, right, summed, grad_conv)
        left = halved(added(left), "sp", 2)
        right = halved(added(right), "sp", 1)
        summed = (summed, swapped(summed, "sp", 0))
    top = conv_backward(grad_conv, None, conv_taps, glu_value, glu_gate, 0)
    if by_halves:
        left, right, summed, top, grad_conv = together(left, right, summed, top, grad_conv)
        both = jnp.concatenate([added(left), added(right)], axis=1)
        both = halved(both, "sp", 3)
        summed = summed[0] + summed[1]
        summed = (summed, swapped(summed, "sp", 1))
    bottom = conv_backward(grad_conv, ahead, conv_taps, glu_value, glu_gate, cut)
    if by_halves:
        both, summed, bottom = together(both, summed, bottom)
        grad_proj = added(both)[0].T
        summed = summed[0] + summed[1]
        for bit in (2, 3):
            summed = summed + swapped(summed, "sp", bit)
    else:
        summed = summed_over(summed, "sp")
    grad_value = jnp.concatenate([top[0], bottom[0]], axis=0)
    grad_gate = jnp.concatenate([top[1], bottom[1]], axis=0)
    return (grad_value, grad_gate, summed[:taps], summed[taps], summed[taps + 1], grad_proj)


def solution(mesh):
    return jax.shard_map(
        on_device,
        mesh=mesh,
        in_specs=(
            P("sp", "tp"),
            P("sp", "tp"),
            P(None, "tp"),
            P("tp"),
            P("tp"),
            P("tp", None),
            P("sp", None),
        ),
        out_specs=(P("sp", "tp"), P("sp", "tp"), P(None, "tp"), P("tp"), P("tp"), P("sp", "tp")),
        check_vma=False,
    )
```

```python
import jax
import jax.numpy as jnp
import numpy as np
from jax import lax
from jax.experimental import pallas as pl
from jax.experimental.pallas import tpu as pltpu
from jax.sharding import PartitionSpec as P

LANES = 128
TILE = 64


def passed_along(shard, axis, by):
    size = lax.axis_size(axis)
    pairs = [(i, i + by) for i in range(size) if 0 <= i + by < size]
    return lax.ppermute(shard, axis, pairs)


def swapped(shard, axis, bit):
    size = lax.axis_size(axis)
    return lax.ppermute(shard, axis, [(i, i ^ (1 << bit)) for i in range(size)])


def bits_of(size):
    bits = size.bit_length() - 1
    return bits if 1 << bits == size else None


def summed_over(shard, axis):
    bits = bits_of(lax.axis_size(axis))
    if bits is None:
        return lax.psum(shard, axis)
    for bit in range(bits):
        shard = shard + swapped(shard, axis, bit)
    return shard


def together(*values):
    return lax.optimization_barrier(values)


def call(body, outs, *args, scalars=0, scratch=()):
    vmem = pl.BlockSpec(memory_space=pltpu.VMEM)
    resident = [pltpu.with_memory_space_constraint(a, pltpu.VMEM) for a in args[scalars:]]
    return pl.pallas_call(
        body,
        in_specs=[pl.BlockSpec(memory_space=pltpu.SMEM)] * scalars + [vmem] * (len(args) - scalars),
        out_specs=[vmem] * len(outs),
        out_shape=[pltpu.VMEM(shape, kind) for shape, kind in outs],
        scratch_shapes=list(scratch),
        compiler_params=pltpu.CompilerParams(vmem_limit_bytes=20 * 1024 * 1024),
    )(*args[:scalars], *resident)


def group(g):
    return slice(g * LANES, (g + 1) * LANES)


def as_row(columns):
    return jnp.sum(columns.T, axis=0, keepdims=True)


def as_column(row):
    return jnp.broadcast_to(row, (LANES, row.shape[1])).T


def conv_forward(value, gate, before, conv_taps):
    rows, width = value.shape
    taps = conv_taps.shape[0]
    pad = before.shape[0]
    groups = width // LANES

    def body(value_ref, gate_ref, before_ref, taps_ref, conv_ref, padded_ref, sums_ref):
        for g in range(groups):
            padded_ref[g, :pad, :] = before_ref[:, group(g)].astype(jnp.float32)
            v = value_ref[:, group(g)].astype(jnp.float32)
            s = jax.nn.sigmoid(gate_ref[:, group(g)].astype(jnp.float32))
            padded_ref[g, pad:, :] = (v * s).astype(jnp.bfloat16).astype(jnp.float32)
        for g in range(groups):
            weights = [taps_ref[k : k + 1, group(g)] for k in range(taps)]

            def tile(n, carry):
                first = pl.multiple_of(n * TILE, TILE)
                total = jnp.zeros((TILE, LANES), jnp.float32)
                for k in range(taps):
                    total = total + weights[k] * padded_ref[
                        g, pl.ds(first + (pad - taps + 1 + k), TILE), :
                    ]
                conv_ref[pl.ds(first, TILE), group(g)] = total
                return carry

            lax.fori_loop(0, rows // TILE, tile, 0)
        total = jnp.zeros((rows, LANES), jnp.float32)
        squares = jnp.zeros((rows, LANES), jnp.float32)
        for g in range(groups):
            c = conv_ref[:, group(g)]
            total = total + c
            squares = squares + c * c
        sums_ref[0:1, :] = as_row(total)
        sums_ref[1:2, :] = as_row(squares)

    return call(
        body,
        [
            ((rows, width), jnp.float32),
            ((groups, rows + pad, LANES), jnp.float32),
            ((2, rows), jnp.float32),
        ],
        value, gate, before, conv_taps,
    )


def statistics(sums_ref, channels):
    mean = sums_ref[0:1, :] / channels
    var = sums_ref[1:2, :] / channels - mean * mean
    return as_column(mean), as_column(lax.rsqrt(var + 1e-05))


def products(me_ref, order, grad_ref, act, block):
    for n in range(0, len(order), 2):
        picked = [
            grad_ref[:, pl.ds(pl.multiple_of((me_ref[0] ^ b) * block, block), block)]
            for b in order[n : n + 2]
        ]
        pair = jnp.dot(
            act, jnp.concatenate(picked, axis=1), preferred_element_type=jnp.float32
        )
        yield n, pair[:, :block]
        yield n + 1, pair[:, block:]


def normed_act(conv, sums, gain, bias, out_grad, me, order, block, channels):
    rows, width = conv.shape
    groups = width // LANES
    count = len(order)

    def body(me_ref, conv_ref, sums_ref, gain_ref, bias_ref, grad_ref, act_ref, sent_ref):
        mean, rstd = statistics(sums_ref, channels)
        for g in range(groups):
            xhat = (conv_ref[:, group(g)] - mean) * rstd
            normed = xhat * gain_ref[:, group(g)] + bias_ref[:, group(g)]
            act = normed * jax.nn.sigmoid(normed)
            act_ref[group(g), :] = act.T.astype(jnp.bfloat16)
        if count:
            for n, product in products(me_ref, order, grad_ref, act_ref[...], block):
                sent_ref[n] = product.astype(jnp.bfloat16)
        else:
            sent_ref[...] = jnp.zeros_like(sent_ref)

    shape = (count, width, block) if count else (16, LANES)
    return call(
        body,
        [((width, rows), jnp.bfloat16), (shape, jnp.bfloat16)],
        me, conv, sums, gain, bias, out_grad,
        scalars=1,
    )


def kept_products(act, out_grad, me, order, block, got):
    width = act.shape[0]
    half = width // 2
    count = len(order)

    def body(me_ref, act_ref, grad_ref, got_ref, kl_ref, sl_ref, kr_ref, sr_ref):
        for n, product in products(me_ref, order, grad_ref, act_ref[...], block):
            product = product + got_ref[n].astype(jnp.float32)
            left, right = product[:half], product[half:]
            first, second, rest = n >> 2, (n >> 1) & 1, n & 1
            if first:
                sl_ref[second * 2 + rest] = left.astype(jnp.bfloat16)
            else:
                kl_ref[second * 2 + rest] = left
            if second:
                sr_ref[first * 2 + rest] = right.astype(jnp.bfloat16)
            else:
                kr_ref[first * 2 + rest] = right

    shape = (count // 2, half, block)
    return call(
        body,
        [(shape, jnp.float32), (shape, jnp.bfloat16)] * 2,
        me, act, out_grad, got,
        scalars=1,
    )


def normed_gradient(conv, sums, gain, bias, upper, lower, channels):
    rows, width = conv.shape
    groups = width // LANES
    cut = upper.shape[0]

    def body(conv_ref, sums_ref, gain_ref, bias_ref, up_ref, low_ref, gx_ref, xhat_ref, row_ref, col_ref):
        mean, rstd = statistics(sums_ref, channels)
        first = jnp.zeros((rows, LANES), jnp.float32)
        second = jnp.zeros((rows, LANES), jnp.float32)
        for g in range(groups):
            xhat = (conv_ref[:, group(g)] - mean) * rstd
            normed = xhat * gain_ref[:, group(g)] + bias_ref[:, group(g)]
            sig = jax.nn.sigmoid(normed)
            ga = jnp.concatenate([up_ref[:, group(g)], low_ref[:, group(g)]], axis=0)
            gn = ga * sig * (1.0 + normed * (1.0 - sig))
            col_ref[0:1, group(g)] = jnp.sum(gn * xhat, axis=0, keepdims=True)
            col_ref[1:2, group(g)] = jnp.sum(gn, axis=0, keepdims=True)
            gx = gn * gain_ref[:, group(g)]
            first = first + gx
            second = second + gx * xhat
            gx_ref[:, group(g)] = gx
            xhat_ref[:, group(g)] = xhat
        row_ref[0:1, :] = as_row(first)
        row_ref[1:2, :] = as_row(second)

    return call(
        body,
        [
            ((rows, width), jnp.float32),
            ((rows, width), jnp.float32),
            ((2, rows), jnp.float32),
            ((2, width), jnp.float32),
        ],
        conv, sums, gain, bias, upper, lower,
    )


def conv_gradient(gx, xhat, sums, terms, channels, pad):
    rows, width = gx.shape
    groups = width // LANES

    def body(gx_ref, xhat_ref, sums_ref, terms_ref, out_ref, edge_ref):
        _, rstd = statistics(sums_ref, channels)
        first = as_column(terms_ref[0:1, :] / channels)
        second = as_column(terms_ref[1:2, :] / channels)
        for g in range(groups):
            out = rstd * (gx_ref[:, group(g)] - first - xhat_ref[:, group(g)] * second)
            out_ref[g] = out
            edge_ref[g] = out[:pad]

    return call(
        body,
        [((groups, rows, LANES), jnp.float32), ((groups, pad, LANES), jnp.float32)],
        gx, xhat, sums, terms,
    )


def taps_gradient(grad_conv, padded, columns, taps):
    groups, rows, _ = grad_conv.shape
    pad = padded.shape[1] - rows
    height = -(-(taps + 2) // 8) * 8

    def body(grad_ref, padded_ref, col_ref, out_ref):
        out_ref[...] = jnp.zeros_like(out_ref)
        out_ref[taps : taps + 2, :] = col_ref[...]
        for g in range(groups):
            def tile(n, totals):
                first = pl.multiple_of(n * 16, 16)
                grad = [grad_ref[g, pl.ds(first + 8 * m, 8), :] for m in range(2)]
                return tuple(
                    totals[k] + sum(
                        grad[m] * padded_ref[g, pl.ds(first + (8 * m + pad - taps + 1 + k), 8), :]
                        for m in range(2)
                    )
                    for k in range(taps)
                )

            totals = lax.fori_loop(
                0, rows // 16, tile, tuple(jnp.zeros((8, LANES), jnp.float32) for _ in range(taps))
            )
            for k in range(taps):
                out_ref[k : k + 1, group(g)] = jnp.sum(totals[k], axis=0, keepdims=True)

    return call(body, [((height, groups * LANES), jnp.float32)], grad_conv, padded, columns)[0]


def conv_backward(grad_conv, ahead, conv_taps, value, gate, start, top=None):
    groups, rows, _ = grad_conv.shape
    taps = conv_taps.shape[0]
    count = rows // 2
    width = groups * LANES
    final = ahead is not None

    def body(*refs):
        if final:
            grad_ref, ahead_ref, taps_ref, value_ref, gate_ref, tv_ref, tg_ref = refs[:7]
            gv_ref, gg_ref, held_ref = refs[7:]
            gv_ref[:start] = tv_ref[...]
            gg_ref[:start] = tg_ref[...]
            held_ref[:, :count, :] = grad_ref[:, start:, :]
            held_ref[:, count:, :] = ahead_ref[...]
            source, base = held_ref, 0
        else:
            grad_ref, taps_ref, value_ref, gate_ref, gv_ref, gg_ref = refs
            source, base = grad_ref, start
        for g in range(groups):
            weights = [taps_ref[k : k + 1, group(g)] for k in range(taps)]

            def tile(n, carry):
                first = pl.multiple_of(n * TILE, TILE)
                total = jnp.zeros((TILE, LANES), jnp.float32)
                for k in range(taps):
                    total = total + weights[k] * source[
                        g, pl.ds(first + (base + taps - 1 - k), TILE), :
                    ]
                here = pl.ds(first + start, TILE)
                v = value_ref[here, group(g)].astype(jnp.float32)
                s = jax.nn.sigmoid(gate_ref[here, group(g)].astype(jnp.float32))
                gv_ref[here, group(g)] = (total * s).astype(jnp.bfloat16)
                gg_ref[here, group(g)] = (total * v * s * (1.0 - s)).astype(jnp.bfloat16)
                return carry

            lax.fori_loop(0, count // TILE, tile, 0)

    outs = [((count, width), jnp.bfloat16)] * 2
    if final:
        scratch = [pltpu.VMEM((groups, count + ahead.shape[1], LANES), jnp.float32)]
        outs = [((rows, width), jnp.bfloat16)] * 2
        return call(body, outs, grad_conv, ahead, conv_taps, value, gate, *top, scratch=scratch)
    return call(body, outs, grad_conv, conv_taps, value, gate)


def halved(blocks, axis, bit):
    count = blocks.shape[0] // 2
    return blocks[:count], swapped(blocks[count:].astype(jnp.bfloat16), axis, bit)


def added(pair):
    return pair[0] + pair[1].astype(jnp.float32)


def on_device(
    glu_value, glu_gate, conv_taps, channel_norm_gain, channel_norm_bias, out_proj, out_grad
):
    rows, width = glu_value.shape
    taps = conv_taps.shape[0]
    pad = -(-(taps - 1) // 16) * 16
    channels = width * lax.axis_size("tp")
    size = lax.axis_size("sp")
    bits = bits_of(size)
    block = out_grad.shape[1] // size
    by_halves = bits == 4 and block % LANES == 0 and width % 256 == 0
    gain, bias = channel_norm_gain[None, :], channel_norm_bias[None, :]
    cut = rows // 2
    me = lax.axis_index("sp").astype(jnp.int32).reshape(1)
    relative = []
    if by_halves:
        relative = [
            sum(((n >> (bits - 2 - b)) & 1) << (b + 1) for b in range(bits - 1))
            for n in range(size // 2)
        ]

    edge = (
        glu_value[rows - pad :].astype(jnp.float32)
        * jax.nn.sigmoid(glu_gate[rows - pad :].astype(jnp.float32))
    ).astype(jnp.bfloat16)
    before = passed_along(edge, "sp", 1)

    def act_gradient(part):
        return lax.dot_general(
            part, out_proj, (((1,), (1,)), ((), ())), preferred_element_type=jnp.float32
        )

    upper = act_gradient(out_grad[:cut])
    before, upper = together(before, upper)
    conv, padded, sums = conv_forward(glu_value, glu_gate, before, conv_taps)
    later, sums = together(out_grad, sums)
    lower = act_gradient(later[cut:])
    sums = summed_over(sums, "tp")
    sums, lower = together(sums, lower)
    act, sent = normed_act(
        conv, sums, gain, bias, out_grad, me, [r + 1 for r in relative], block, channels
    )
    if by_halves:
        got = swapped(sent, "sp", 0)
        sums, act = together(sums, act)
    gx, xhat, row_terms, column_terms = normed_gradient(
        conv, sums, gain, bias, upper, lower, channels
    )
    terms = summed_over(row_terms, "tp")
    if by_halves:
        got, row_terms = together(got, row_terms)
        kl, sl, kr, sr = kept_products(act, out_grad, me, relative, block, got)
        left = (kl, swapped(sl, "sp", 1))
        right = (kr, swapped(sr, "sp", 2))
        terms, kl = together(terms, kl)
        left = (kl, left[1])
    else:
        grad_proj = lax.psum_scatter(
            lax.dot_general(
                out_grad, act, (((0,), (1,)), ((), ())), preferred_element_type=jnp.float32
            ),
            "sp",
            scatter_dimension=0,
            tiled=True,
        )
    grad_conv, edge_gradient = conv_gradient(gx, xhat, sums, terms, channels, pad)
    ahead = passed_along(edge_gradient, "sp", -1)
    summed = taps_gradient(grad_conv, padded, column_terms, taps)
    if by_halves:
        left, right, summed, grad_conv = together(left, right, summed, grad_conv)
        left = halved(added(left), "sp", 2)
        right = halved(added(right), "sp", 1)
        summed = (summed, swapped(summed, "sp", 0))
    top = conv_backward(grad_conv, None, conv_taps, glu_value, glu_gate, 0)
    if by_halves:
        left, right, summed, top, grad_conv = together(left, right, summed, top, grad_conv)
        both = jnp.concatenate([added(left), added(right)], axis=1)
        both = halved(both, "sp", 3)
        summed = summed[0] + summed[1]
        summed = (summed, swapped(summed, "sp", 1))
    bottom = conv_backward(grad_conv, ahead, conv_taps, glu_value, glu_gate, cut, top)
    if by_halves:
        both, summed, bottom = together(both, summed, bottom)
        grad_proj = added(both)[0].T
        summed = summed[0] + summed[1]
        for bit in (2, 3):
            summed = summed + swapped(summed, "sp", bit)
    else:
        summed = summed_over(summed, "sp")
    return (bottom[0], bottom[1], summed[:taps], summed[taps], summed[taps + 1], grad_proj)


def solution(mesh):
    return jax.shard_map(
        on_device,
        mesh=mesh,
        in_specs=(
            P("sp", "tp"),
            P("sp", "tp"),
            P(None, "tp"),
            P("tp"),
            P("tp"),
            P("tp", None),
            P("sp", None),
        ),
        out_specs=(P("sp", "tp"), P("sp", "tp"), P(None, "tp"), P("tp"), P("tp"), P("sp", "tp")),
        check_vma=False,
    )
```
